1024 devices in a mesh: rep: 4 (over z_hi), fs: 32 (over z_lo, y), tp: 8 (over x, core).
Axes of the slice: x: 4, y: 4, z: 32 (z_hi: 4, z_lo: 8; z = z_hi * 8 + z_lo), core: 2. Of those that a mesh axis runs over, the one named last changes fastest.
Arguments:
- stream: bfloat16 [32768, 2048], P(('rep', 'fs')), may hold values from -6 to 6
- gain_mix: float32 [2048], replicated, may hold values from 0.1 to 1.9
- w_query: float32 [2048, 2048], P('fs', 'tp'), may hold values from -0.125 to 0.125
- scale_query: float32 [2048], P('tp'), may hold values from 0.5 to 2
- w_key: float32 [2048, 2048], P('fs', 'tp'), may hold values from -0.125 to 0.125
- scale_key: float32 [2048], P('tp'), may hold values from 0.5 to 2
- w_value: float32 [2048, 2048], P('fs', 'tp'), may hold values from -0.125 to 0.125
- scale_value: float32 [2048], P('tp'), may hold values from 0.5 to 2
- gain_ffn: float32 [2048], replicated, may hold values from 0.1 to 1.9
- w_gate: float32 [2048, 2816], P('fs', 'tp'), may hold values from -0.125 to 0.125
- scale_gate: float32 [2816], P('tp'), may hold values from 0.5 to 2
- w_up: float32 [2048, 2816], P('fs', 'tp'), may hold values from -0.125 to 0.125
- scale_up: float32 [2816], P('tp'), may hold values from 0.5 to 2
- w_down: float32 [2048, 2816], P('fs', 'tp'), may hold values from -0.109375 to 0.109375
- scale_down: float32 [2048], P('fs'), may hold values from 0.5 to 2
Outputs:
- layer_out: bfloat16 [32768, 2048], P(('rep', 'fs', 'tp'))
The draws below stay inside these ranges and needn't reach their ends.
All inputs are finite; a program needn't handle non-finite values.
Results may differ from the reference program's by a relative error of at most 0.015.
Values may be sent and summed in bfloat16 or wider, within the bound.
No kernel may reach another device: no remote copies, remote signals or barrier semaphores. Data moves between devices by JAX's collectives and lax.ppermute only.
A program may use at most 32 MiB of HBM per device.

```python
import math
import jax
import jax.numpy as jnp
from jax import lax

D = 2048
HEADS = 8
DK = 256
DV = 256
FF = 2816
LEN = 128
BLK = 64
TOKENS = 32768
N_TP = 8


def block_scale(stream_key, shape, pieces, smallest, top_value):
    factor_of = 1.0
    for position, parts in pieces:
        heights = jax.random.uniform(jax.random.fold_in(jax.random.fold_in(stream_key, 6), position), (parts,), jnp.float32, smallest / len(pieces), top_value / len(pieces))
        factor_of = factor_of * jnp.repeat(jnp.exp(heights), shape[position] // parts).reshape((-1,) + (1,) * (len(shape) - 1 - position))
    return factor_of


def scatter_about(rng, extent, width, reach, cuts=(), kind=jnp.bfloat16):
    level = block_scale(rng, extent, cuts, -0.22, 0.18) if cuts else 1.0
    drawn = jax.random.normal(rng, extent, jnp.float32) * width * level
    return jnp.minimum(jnp.maximum(drawn, -reach), reach).astype(kind)


def setup_inputs(seed: int = 0) -> dict:
    arg_keys = jax.random.split(jax.random.key(seed), 16)
    return {
        "stream": scatter_about(arg_keys[0], (TOKENS, D), 1.0, 6.0, ((0, 128),)),
        "gain_mix": jnp.clip(1.0 + 0.18 * jax.random.normal(arg_keys[1], (D,), jnp.float32), 0.1, 1.9),
        "w_query": scatter_about(arg_keys[2], (D, HEADS * DK), D ** -0.5, 0.125, ((0, 32), (1, 8)), jnp.float32),
        "scale_query": jnp.clip(jnp.exp(math.log(2.0) - 1.3862944 * jax.random.uniform(arg_keys[3], (HEADS * DK,), jnp.float32) ** block_scale(arg_keys[3], (HEADS * DK,), ((0, 8),), -0.2, 0.2)), 0.5, 2.0),
        "w_key": scatter_about(arg_keys[4], (D, HEADS * DK), D ** -0.5, 0.125, ((0, 32), (1, 8)), jnp.float32),
        "scale_key": jnp.clip(jnp.exp(math.log(2.0) - 1.3862944 * jax.random.uniform(arg_keys[5], (HEADS * DK,), jnp.float32) ** block_scale(arg_keys[5], (HEADS * DK,), ((0, 8),), -0.2, 0.2)), 0.5, 2.0),
        "w_value": scatter_about(arg_keys[6], (D, HEADS * DV), D ** -0.5, 0.125, ((0, 32), (1, 8)), jnp.float32),
        "scale_value": jnp.clip(jnp.exp(math.log(2.0) - 1.3862944 * jax.random.uniform(arg_keys[7], (HEADS * DV,), jnp.float32) ** block_scale(arg_keys[7], (HEADS * DV,), ((0, 8),), -0.2, 0.2)), 0.5, 2.0),
        "gain_ffn": jnp.clip(1.0 + 0.18 * jax.random.normal(arg_keys[8], (D,), jnp.float32), 0.1, 1.9),
        "w_gate": scatter_about(arg_keys[9], (D, FF), D ** -0.5, 0.125, ((0, 32), (1, 8)), jnp.float32),
        "scale_gate": jnp.clip(jnp.exp(math.log(2.0) - 1.3862944 * jax.random.uniform(arg_keys[10], (FF,), jnp.float32) ** block_scale(arg_keys[10], (FF,), ((0, 8),), -0.2, 0.2)), 0.5, 2.0),
        "w_up": scatter_about(arg_keys[11], (D, FF), D ** -0.5, 0.125, ((0, 32), (1, 8)), jnp.float32),
        "scale_up": jnp.clip(jnp.exp(math.log(2.0) - 1.3862944 * jax.random.uniform(arg_keys[12], (FF,), jnp.float32) ** block_scale(arg_keys[12], (FF,), ((0, 8),), -0.2, 0.2)), 0.5, 2.0),
        "w_down": scatter_about(arg_keys[13], (D, FF), FF ** -0.5, 0.109375, ((0, 32), (1, 8)), jnp.float32),
        "scale_down": jnp.clip(jnp.exp(math.log(2.0) - 1.3862944 * jax.random.uniform(arg_keys[14], (D,), jnp.float32) ** block_scale(arg_keys[14], (D,), ((0, 32),), -0.2, 0.2)), 0.5, 2.0),
    }


EPS = 1e-06
THETA = 10000.0
HIGH = lax.Precision.HIGHEST

def rms_scale(values):
    return lax.rsqrt(lax.optimization_barrier(jnp.mean(values * values, axis=-1, keepdims=True)) + EPS)

def head_scale(values):
    return 1.0 / jnp.maximum(jnp.sqrt(lax.optimization_barrier(jnp.mean(values * values, axis=-1, keepdims=True))), 1.0)

def rotate(heads_data, positions):
    half = heads_data.shape[-1] // 2
    frequency = THETA ** (-(jnp.arange(half, dtype=jnp.float32) / half))
    angle = positions.astype(jnp.float32)[:, None, None] * frequency
    cosine = jnp.cos(angle)
    sine = jnp.sin(angle)
    first = heads_data[..., :half]
    second = heads_data[..., half:]
    return jnp.concatenate([first * cosine - second * sine, second * cosine + first * sine], axis=-1)

def retention_blocks(queries, keys, values, log_decay):
    total_rows, heads, key_width = queries.shape
    value_width = values.shape[-1]
    queries = queries.reshape((-1, LEN // BLK, BLK, heads, key_width))
    keys = keys.reshape((-1, LEN // BLK, BLK, heads, key_width))
    values = values.reshape((-1, LEN // BLK, BLK, heads, value_width))
    offsets = jnp.arange(BLK, dtype=jnp.float32)
    distance = offsets[:, None] - offsets[None, :]
    decay_mask = jnp.where(distance >= 0, jnp.exp(log_decay[:, None, None] * jnp.maximum(distance, 0.0)), 0.0)
    scores = jnp.einsum('snihd,snjhd->snhij', queries, keys, precision=HIGH) * decay_mask
    inner = jnp.einsum('snhij,snjhe->snihe', scores, values, precision=HIGH)
    query_decay = jnp.exp(log_decay[None, :] * (offsets[:, None] + 1.0))[:, :, None]
    key_decay = jnp.exp(log_decay[None, :] * (BLK - 1.0 - offsets[:, None]))[:, :, None]
    block_decay = jnp.exp(log_decay * BLK)[None, :, None, None]

    def advance(state, inputs):
        block_query, block_key, block_value = inputs
        carried = jnp.einsum('sihd,shde->sihe', block_query, state, precision=HIGH)
        state = state * block_decay + jnp.einsum('sjhd,sjhe->shde', block_key, block_value, precision=HIGH)
        return (state, carried)
    moved = (jnp.moveaxis(queries * query_decay, 1, 0), jnp.moveaxis(keys * key_decay, 1, 0), jnp.moveaxis(values, 1, 0))
    initial = jnp.zeros((queries.shape[0], heads, key_width, value_width), jnp.float32)
    _, carried = lax.scan(advance, initial, moved)
    return (inner + jnp.moveaxis(carried, 0, 1)).reshape(total_rows, heads, value_width)

def reference(stream, gain_mix, w_query, scale_query, w_key, scale_key, w_value, scale_value, gain_ffn, w_gate, scale_gate, w_up, scale_up, w_down, scale_down):
    stream_f = stream.astype(jnp.float32)
    normed = (stream_f * rms_scale(stream_f) * gain_mix).astype(jnp.bfloat16)

    def project(weight, scale):
        return (jnp.dot(normed, weight.astype(jnp.bfloat16), preferred_element_type=jnp.float32) * scale).astype(jnp.bfloat16)
    query = project(w_query, scale_query)
    key = project(w_key, scale_key)
    value = project(w_value, scale_value)
    total_rows = stream.shape[0]
    positions = jnp.arange(total_rows, dtype=jnp.int32) % LEN
    queries = rotate(query.astype(jnp.float32).reshape(total_rows, HEADS, DK), positions)
    keys = rotate(key.astype(jnp.float32).reshape(total_rows, HEADS, DK), positions) * DK ** (-0.5)
    values = value.astype(jnp.float32).reshape(total_rows, HEADS, DV)
    log_decay = jnp.log(1.0 - jnp.power(2.0, -5.0 - jnp.arange(HEADS, dtype=jnp.float32)))
    retained = retention_blocks(queries, keys, values, log_decay)
    mixed = (retained * head_scale(retained)).astype(jnp.bfloat16).reshape(total_rows, HEADS * DV)
    resid = stream_f + mixed.astype(jnp.float32)
    normed_ffn = (resid * rms_scale(resid) * gain_ffn).astype(jnp.bfloat16)
    gate = jnp.dot(normed_ffn, w_gate.astype(jnp.bfloat16), preferred_element_type=jnp.float32) * scale_gate
    upward = jnp.dot(normed_ffn, w_up.astype(jnp.bfloat16), preferred_element_type=jnp.float32) * scale_up
    hidden = (jax.nn.silu(gate) * upward).astype(jnp.bfloat16)
    down_rounded = w_down.astype(jnp.bfloat16)
    block_width = FF // N_TP
    channel_out = jnp.zeros((total_rows, D), jnp.float32)
    for number in range(N_TP):
        piece = hidden[:, number * block_width:(number + 1) * block_width]
        columns = down_rounded[:, number * block_width:(number + 1) * block_width]
        partial_sum = lax.dot_general(piece, columns, (((1,), (1,)), ((), ())), preferred_element_type=jnp.float32) * scale_down
        partial_sum = lax.optimization_barrier(partial_sum.astype(jnp.bfloat16))
        channel_out = channel_out + partial_sum.astype(jnp.float32)
    return (resid + channel_out).astype(jnp.bfloat16)
```

```python
import jax
import jax.numpy as jnp
import numpy as np
from jax import lax
from jax.experimental import pallas as pl
from jax.experimental.pallas import tpu as pltpu
from jax.sharding import Mesh
from jax.sharding import PartitionSpec as P

EPS = 1e-06
THETA = 10000.0
HIGH = lax.Precision.HIGHEST
LEN = 128
Z = ("zh", "zl")
TP = ("x", "c")
F32 = jnp.float32
BF16 = jnp.bfloat16
VMEM = pl.BlockSpec(memory_space=pltpu.VMEM)
SMEM = pl.BlockSpec(memory_space=pltpu.SMEM)
MIB = 1 << 20


def shift(array, axis, offset):
    n = lax.axis_size(axis)
    return lax.ppermute(array, axis, [((i + offset) % n, i) for i in range(n)])


def call(kernel, out_shape, *args, scratch=(), specs=None, limit=24):
    return pl.pallas_call(
        kernel,
        out_shape=out_shape,
        in_specs=specs or [VMEM] * len(args),
        out_specs=jax.tree.map(lambda _: VMEM, out_shape),
        scratch_shapes=list(scratch),
        compiler_params=pltpu.CompilerParams(vmem_limit_bytes=limit * MIB),
    )(*args)


def pack_kernel(wq, wk, wv, wg, wu, wd, sd, qkv, ffn):
    qkv[:, 0:256] = wq[...].astype(BF16)
    qkv[:, 256:512] = wk[...].astype(BF16)
    qkv[:, 512:768] = wv[...].astype(BF16)
    ffn[0:64, :] = jnp.zeros((64, 768), BF16)
    ffn[0:64, 0:352] = wg[...].astype(BF16)
    ffn[0:64, 384:736] = wu[...].astype(BF16)
    scale = sd[...]
    high = scale.astype(BF16).astype(F32)
    middle = (scale - high).astype(BF16).astype(F32)
    low = scale - high - middle
    lane = lax.broadcasted_iota(jnp.int32, (64, 384), 1)
    extra = jnp.where(lane == 352, high, jnp.where(lane == 353, middle, jnp.where(lane == 354, low, 0.0)))
    extra = extra.astype(BF16)
    ffn[64:96, 0:384] = extra[0:32]
    ffn[64:96, 384:768] = extra[32:64]
    down = wd[...].astype(BF16)
    ffn[64:96, 0:352] = down[0:32]
    ffn[64:96, 384:736] = down[32:64]


def retention_kernel(where, decay, normed, own, p1, m1, p2, m2, p3, m3, p4, m4, sq, sk, sv, cosine, sine, out):
    zl = where[0]
    acc = jnp.zeros((256, 768), F32)
    far = jnp.concatenate([p4[...], m4[0:80, :]], axis=0)
    blocks = {0: own, 1: p1, -1: m1, 2: p2, -2: m2, 3: p3, -3: m3}
    for k in (0, 1, -1, 2, -2, 3, -3, 4):
        block = lax.rem(zl + k + 8, 8)
        rows = normed[:, pl.ds(pl.multiple_of(block * 256, 256), 256)]
        weight = far if k == 4 else blocks[k][0:256, :]
        acc = acc + jnp.dot(rows, weight, preferred_element_type=F32)
    query = (acc[:, 0:256] * sq[...]).astype(BF16).astype(F32)
    key = (acc[:, 256:512] * sk[...]).astype(BF16).astype(F32)
    value = (acc[:, 512:768] * sv[...]).astype(BF16).astype(F32)
    cos = cosine[...]
    sin = sine[...]
    distance = lax.broadcasted_iota(jnp.int32, (LEN, LEN), 0) - lax.broadcasted_iota(jnp.int32, (LEN, LEN), 1)
    distance = distance.astype(F32)
    mask = jnp.where(distance >= 0, jnp.exp(decay[0] * jnp.maximum(distance, 0.0)), 0.0)

    def rotate(values):
        first, second = values[:, 0:128], values[:, 128:256]
        return jnp.concatenate([first * cos - second * sin, second * cos + first * sin], axis=1)

    for s in range(2):
        rows = slice(s * LEN, (s + 1) * LEN)
        rot_query = rotate(query[rows])
        rot_key = rotate(key[rows]) * (256**-0.5)
        scores = lax.dot_general(
            rot_query, rot_key, (((1,), (1,)), ((), ())), precision=HIGH, preferred_element_type=F32
        )
        retained = jnp.dot(scores * mask, value[rows], precision=HIGH, preferred_element_type=F32)
        square = jnp.mean(retained * retained, axis=-1, keepdims=True)
        mixed = (retained * (1.0 / jnp.maximum(jnp.sqrt(square), 1.0))).astype(BF16)
        for copy in range(4):
            out[copy, rows, :] = mixed


def ffn_kernel(
    where, stream, mixed, gain, own, p1, m1, p2, m2, p3, m3, m4,
    ap, am, a2p, a2m, bp, bm, b2p, b2m, sg, su, out, own_rows, resid
):
    zl, y, tp = where[0], where[1], where[2]
    total = jnp.zeros((256, 1), F32)
    for b in range(8):
        rows = stream[:, b * 256 : (b + 1) * 256].astype(F32) + mixed[b % 2, b // 2].astype(F32)
        resid[b] = rows
        total = total + jnp.sum(rows * rows, axis=-1, keepdims=True)
        own_rows[:, b * 256 : (b + 1) * 256] = resid[b, pl.ds(pl.multiple_of(tp * 32, 32), 32), :]
    inverse = lax.rsqrt(total * (1.0 / 2048) + EPS)
    near = {0: own, 1: p1, -1: m1, 2: p2, -2: m2, 3: p3, -3: m3}
    places = {0: ("a", 0), 1: ("a", 1), -1: ("a", 2), 2: ("a", 3), -2: ("a", 4), 3: ("b", 0), -3: ("b", 1), 4: ("b", 2)}

    def shard(k, j, start, stop):
        if j == 0:
            return m4[80 + start : 80 + stop, :] if k == 4 else near[k][256 + start : 256 + stop, :]
        batch, place = places[k]
        if j in (1, 3):
            ref = {("a", 1): ap, ("a", 3): am, ("b", 1): bp, ("b", 3): bm}[batch, j]
            return ref[place * 96 + start : place * 96 + stop, :]
        half = 240 if batch == "a" else 144
        first, second = (a2p, a2m) if batch == "a" else (b2p, b2m)
        low, high = place * 96 + start, place * 96 + stop
        if high <= half:
            return first[low:high, :]
        if low >= half:
            return second[low - half : high - half, :]
        return jnp.concatenate([first[low:half, :], second[0 : high - half, :]], axis=0)

    def turned(values, by_one, by_two):
        values = jnp.where(by_one, pltpu.roll(values, 192, 1), values)
        return jnp.where(by_two, pltpu.roll(values, 128, 1), values)

    acc = jnp.zeros((256, 768), F32)
    order = (0, 1, -1, 2, -2, 3, -3, 4)
    for k in order:
        block = lax.rem(zl + k + 8, 8)
        rows = turned(resid[block] * inverse * gain[block], y % 2 == 1, y >= 2).astype(BF16)
        weight = jnp.concatenate([shard(k, j, 0, 64) for j in range(4)], axis=0)
        acc = acc + jnp.dot(rows, weight, preferred_element_type=F32)
    gate = acc[:, 0:384] * sg[...]
    hidden = (gate / (1.0 + jnp.exp(-gate)) * (acc[:, 384:768] * su[...])).astype(BF16)
    lane = lax.broadcasted_iota(jnp.int32, (16, 384), 1)
    pick = jnp.where((lane >= 352) & (lane <= 354), 1.0, 0.0).astype(BF16)
    for place, k in enumerate(order):
        pieces = []
        for j in range(4):
            piece = shard(k, j, 64, 96)
            pieces += [piece[:, 0:384], piece[:, 384:768]]
        weight = jnp.concatenate(pieces, axis=0)
        across = (((1,), (1,)), ((), ()))
        scale = lax.dot_general(pick, weight, across, preferred_element_type=F32)
        partial = lax.dot_general(hidden, weight, across, preferred_element_type=F32)
        out[:, place * 256 : (place + 1) * 256] = (partial * scale[0:1, :]).astype(BF16)


def finish_kernel(where, arrived, own_rows, out):
    zl, y = where[0], where[1]
    for place, k in enumerate((0, 1, -1, 2, -2, 3, -3, 4)):
        block = lax.rem(zl + k + 8, 8)
        columns = pl.ds(pl.multiple_of(block * 256, 256), 256)
        total = jnp.zeros((32, 256), F32)
        for i in range(8):
            total = total + arrived[i, :, place * 256 : (place + 1) * 256].astype(F32)
        total = jnp.where(y % 2 == 1, pltpu.roll(total, 64, 1), total)
        total = jnp.where(y >= 2, pltpu.roll(total, 128, 1), total)
        out[:, columns] = (own_rows[:, columns] + total).astype(BF16)


def shards(
    stream, gain_mix, w_query, scale_query, w_key, scale_key, w_value, scale_value,
    gain_ffn, w_gate, scale_gate, w_up, scale_up, w_down, scale_down,
):
    tp = lax.axis_index(TP)
    where = jnp.stack([lax.axis_index("zl"), lax.axis_index("y"), tp]).astype(jnp.int32)
    qkv, ffn = call(
        pack_kernel,
        (jax.ShapeDtypeStruct((64, 768), BF16), jax.ShapeDtypeStruct((96, 768), BF16)),
        w_query, w_key, w_value, w_gate, w_up, w_down, scale_down[:, None],
    )
    own = jnp.concatenate([lax.all_gather(qkv, "y", axis=0, tiled=True), ffn], axis=0)
    p1, m1 = shift(own, Z, 1), shift(own, Z, -1)
    p2, m2 = shift(p1, Z, 1), shift(m1, Z, -1)
    p3, m3 = shift(p2, Z, 1), shift(m2, Z, -1)
    p4, m4 = shift(p3[0:176], Z, 1), shift(m3[176:352], Z, -1)

    def along_y(batch):
        half = batch.shape[0] // 2
        plus, minus = shift(batch, "y", 1), shift(batch, "y", -1)
        return plus, minus, shift(plus[:half], "y", 1), shift(minus[half:], "y", -1)

    batch_a = jnp.concatenate([own[256:], p1[256:], m1[256:], p2[256:], m2[256:]], axis=0)
    batch_b = jnp.concatenate([p3[256:], m3[256:], m4[80:]], axis=0)
    far_a = along_y(batch_a)
    far_b = along_y(batch_b)

    stream_f = stream.astype(F32)
    square = jnp.mean(stream_f * stream_f, axis=-1, keepdims=True)
    normed = (stream_f * lax.rsqrt(square + EPS) * gain_mix).astype(BF16)
    angle = np.arange(LEN)[:, None] * THETA ** (-(np.arange(128) / 128))
    cosine, sine = jnp.asarray(np.cos(angle), F32), jnp.asarray(np.sin(angle), F32)
    decay = jnp.log(1.0 - jnp.power(2.0, -5.0 - tp.astype(F32)))[None]
    mixed = call(
        retention_kernel,
        jax.ShapeDtypeStruct((4, 256, 256), BF16),
        where, decay, normed, own, p1, m1, p2, m2, p3, m3, p4, m4,
        scale_query[None], scale_key[None], scale_value[None], cosine, sine,
        specs=[SMEM, SMEM] + [VMEM] * 15,
    )
    mixed = lax.all_to_all(mixed, "x", split_axis=0, concat_axis=0, tiled=True)
    mixed = lax.all_gather(mixed, "c")
    wide = lambda scale: jnp.pad(scale, (0, 32))[None]
    partial, own_rows = call(
        ffn_kernel,
        (jax.ShapeDtypeStruct((256, 2048), BF16), jax.ShapeDtypeStruct((32, 2048), F32)),
        where, stream, mixed, gain_ffn.reshape(8, 1, 256), own, p1, m1, p2, m2, p3, m3, m4,
        *far_a, *far_b, wide(scale_gate), wide(scale_up),
        scratch=[pltpu.VMEM((8, 256, 256), F32)],
        specs=[SMEM] + [VMEM] * 21,
    )
    arrived = lax.all_to_all(partial.reshape(8, 32, 2048), TP, split_axis=0, concat_axis=0, tiled=True)
    return call(
        finish_kernel, jax.ShapeDtypeStruct((32, 2048), BF16), where, arrived, own_rows, specs=[SMEM] + [VMEM] * 2
    )


def solution(mesh):
    torus = Mesh(
        mesh.devices.reshape(mesh.shape["rep"], mesh.shape["fs"] // 4, 4, 4, 2),
        ("zh", "zl", "y", "x", "c"),
    )
    rows, weight, columns = P(("zh", "zl", "y"), None), P(("zl", "y"), TP), P(TP)
    in_specs = (
        rows, P(), weight, columns, weight, columns, weight, columns,
        P(), weight, columns, weight, columns, weight, P(("zl", "y")),
    )
    return jax.shard_map(
        shards, mesh=torus, in_specs=in_specs, out_specs=P(("zh", "zl", "y", "x", "c"), None), check_vma=False
    )
```

```python
import jax
import jax.numpy as jnp
import numpy as np
from jax import lax
from jax.experimental import pallas as pl
from jax.experimental.pallas import tpu as pltpu
from jax.sharding import Mesh
from jax.sharding import PartitionSpec as P


EPS = 1e-06
THETA = 10000.0
HIGH = lax.Precision.HIGHEST
LEN = 128
Z = ("zh", "zl")
TP = ("x", "c")
F32 = jnp.float32
BF16 = jnp.bfloat16
VMEM = pl.BlockSpec(memory_space=pltpu.VMEM)
SMEM = pl.BlockSpec(memory_space=pltpu.SMEM)
MIB = 1 << 20


def shift(array, axis, offset):
    n = lax.axis_size(axis)
    return lax.ppermute(array, axis, [((i + offset) % n, i) for i in range(n)])


def call(kernel, out_shape, *args, scratch=(), specs=None, limit=6):
    return pl.pallas_call(
        kernel,
        out_shape=out_shape,
        in_specs=specs or [VMEM] * len(args),
        out_specs=jax.tree.map(lambda _: VMEM, out_shape),
        scratch_shapes=list(scratch),
        compiler_params=pltpu.CompilerParams(vmem_limit_bytes=limit * MIB),
    )(*args)


def pack_kernel(*refs):
    sources, qkv, ffn, held, sems = refs[:7], refs[7], refs[8], refs[9:16], refs[16]
    copies = [pltpu.make_async_copy(sources[i], held[i], sems.at[i]) for i in range(7)]
    for copy in copies:
        copy.start()
    copies[6].wait()
    diagonal = lax.broadcasted_iota(jnp.int32, (64, 64), 0) == lax.broadcasted_iota(jnp.int32, (64, 64), 1)
    scale = jnp.sum(jnp.where(diagonal, held[6][...], 0.0), axis=1, keepdims=True)
    high = scale.astype(BF16).astype(F32)
    middle = (scale - high).astype(BF16).astype(F32)
    low = scale - high - middle
    lane = lax.broadcasted_iota(jnp.int32, (64, 384), 1)
    extra = jnp.where(lane == 352, high, jnp.where(lane == 353, middle, jnp.where(lane == 354, low, 0.0)))
    extra = extra.astype(BF16)
    ffn[0:64, :] = jnp.zeros((64, 768), BF16)
    ffn[64:96, 0:384] = extra[0:32]
    ffn[64:96, 384:768] = extra[32:64]
    for copy in copies[:6]:
        copy.wait()
    wq, wk, wv, wg, wu, wd = held[:6]
    for copy in range(4):
        qkv[copy, :, 0:256] = wq[...].astype(BF16)
        qkv[copy, :, 256:512] = wk[...].astype(BF16)
        qkv[copy, :, 512:768] = wv[...].astype(BF16)
    ffn[0:64, 0:352] = wg[...].astype(BF16)
    ffn[0:64, 384:736] = wu[...].astype(BF16)
    down = wd[...].astype(BF16)
    ffn[64:96, 0:352] = down[0:32]
    ffn[64:96, 384:736] = down[32:64]


def first_kernel(qkv, fp1, fm1, plus, minus):
    plus[0:256, :] = qkv[...]
    plus[256:352, :] = fp1[...]
    minus[0:256, :] = qkv[...]
    minus[256:304, :] = fm1[48:96, :]
    minus[304:352, :] = fm1[0:48, :]


def batch_a_kernel(own, fp1, fm1, p1, m1, out):
    out[0:96, :] = own[...]
    out[96:192, :] = fp1[...]
    out[192:288, :] = fm1[...]
    out[288:384, :] = p1[256:352, :]
    out[384:432, :] = m1[304:352, :]
    out[432:480, :] = m1[256:304, :]


def batch_b_kernel(p2, m2, p3, m3, ap, am, plus, minus):
    for out in (plus, minus):
        out[0:96, :] = p2[256:352, :]
        out[96:144, :] = m2[304:352, :]
        out[144:192, :] = m2[256:304, :]
        out[192:240, :] = p3[256:304, :]
        out[240:288, :] = m3[256:304, :]
    plus[288:528, :] = ap[0:240, :]
    minus[288:528, :] = am[240:480, :]


def retention_kernel(decays, normed, own, p1, m1, p2, m2, p3, m3, p4, m4, sq, sk, sv, cosine, sine, out):
    zl = lax.axis_index("zl")
    decay = decays[lax.axis_index(TP)]
    acc = jnp.zeros((256, 768), F32)
    far = jnp.concatenate([p4[...], m4[...]], axis=0)
    blocks = {0: own, 1: p1, -1: m1, 2: p2, -2: m2, 3: p3, -3: m3}
    for k in (0, 1, -1, 2, -2, 3, -3, 4):
        block = lax.rem(zl + k + 8, 8)
        rows = normed[:, pl.ds(pl.multiple_of(block * 256, 256), 256)]
        weight = far if k == 4 else blocks[k][0:256, :]
        acc = acc + jnp.dot(rows, weight, preferred_element_type=F32)
    query = (acc[:, 0:256] * sq[...]).astype(BF16).astype(F32)
    key = (acc[:, 256:512] * sk[...]).astype(BF16).astype(F32)
    value = (acc[:, 512:768] * sv[...]).astype(BF16).astype(F32)
    cos = cosine[...]
    sin = sine[...]
    distance = lax.broadcasted_iota(jnp.int32, (LEN, LEN), 0) - lax.broadcasted_iota(jnp.int32, (LEN, LEN), 1)
    distance = distance.astype(F32)
    mask = jnp.where(distance >= 0, jnp.exp(decay * jnp.maximum(distance, 0.0)), 0.0)

    def rotate(values):
        first, second = values[:, 0:128], values[:, 128:256]
        return jnp.concatenate([first * cos - second * sin, second * cos + first * sin], axis=1)

    for s in range(2):
        rows = slice(s * LEN, (s + 1) * LEN)
        rot_query = rotate(query[rows])
        rot_key = rotate(key[rows]) * (256**-0.5)
        scores = lax.dot_general(
            rot_query, rot_key, (((1,), (1,)), ((), ())), precision=HIGH, preferred_element_type=F32
        )
        retained = jnp.dot(scores * mask, value[rows], precision=HIGH, preferred_element_type=F32)
        square = jnp.mean(retained * retained, axis=-1, keepdims=True)
        mixed = (retained * (1.0 / jnp.maximum(jnp.sqrt(square), 1.0))).astype(BF16)
        out[rows, :] = mixed


def ffn_kernel(
    stream, first_heads, last_heads, gain, a0, ap, am, b0, bp, bm, b2p, b2m, sg, su, out, own_rows, resid
):
    zl, y, tp = lax.axis_index("zl"), lax.axis_index("y"), lax.axis_index(TP)
    total = jnp.zeros((256, 1), F32)
    for b in range(8):
        head = (first_heads if b < 4 else last_heads)[b % 2, b // 2 % 2]
        rows = stream[:, b * 256 : (b + 1) * 256].astype(F32) + head.astype(F32)
        resid[b] = rows
        total = total + jnp.sum(rows * rows, axis=-1, keepdims=True)
        own_rows[:, b * 256 : (b + 1) * 256] = resid[b, pl.ds(pl.multiple_of(tp * 32, 32), 32), :]
    inverse = lax.rsqrt(total * (1.0 / 2048) + EPS)
    places = {0: ("a", 0), 1: ("a", 1), -1: ("a", 2), 2: ("a", 3), -2: ("a", 4), 3: ("b", 0), -3: ("b", 1), 4: ("b", 2)}

    def shard(k, j, start, stop):
        batch, place = places[k]
        low, high = place * 96 + start, place * 96 + stop
        if j != 2:
            refs = {"a": {0: a0, 1: ap, 3: am}, "b": {0: b0, 1: bp, 3: bm}}
            return refs[batch][j][low:high, :]
        half, base = (240, 288) if batch == "a" else (144, 0)
        first, second = (bp, bm) if batch == "a" else (b2p, b2m)
        if high <= half:
            return first[base + low : base + high, :]
        if low >= half:
            return second[base + low - half : base + high - half, :]
        return jnp.concatenate([first[base + low : base + half, :], second[base : base + high - half, :]], axis=0)

    def turned(values, by_one, by_two):
        values = jnp.where(by_one, pltpu.roll(values, 192, 1), values)
        return jnp.where(by_two, pltpu.roll(values, 128, 1), values)

    acc = jnp.zeros((256, 768), F32)
    order = (0, 1, -1, 2, -2, 3, -3, 4)
    for k in order:
        block = lax.rem(zl + k + 8, 8)
        rows = turned(resid[block] * inverse * gain[block], y % 2 == 1, y >= 2).astype(BF16)
        weight = jnp.concatenate([shard(k, j, 0, 64) for j in range(4)], axis=0)
        acc = acc + jnp.dot(rows, weight, preferred_element_type=F32)
    gate = acc[:, 0:384] * sg[...]
    hidden = (gate / (1.0 + jnp.exp(-gate)) * (acc[:, 384:768] * su[...])).astype(BF16)
    lane = lax.broadcasted_iota(jnp.int32, (16, 384), 1)
    pick = jnp.where((lane >= 352) & (lane <= 354), 1.0, 0.0).astype(BF16)
    for place, k in enumerate(order):
        pieces = []
        for j in range(4):
            piece = shard(k, j, 64, 96)
            pieces += [piece[:, 0:384], piece[:, 384:768]]
        weight = jnp.concatenate(pieces, axis=0)
        across = (((1,), (1,)), ((), ()))
        scale = lax.dot_general(pick, weight, across, preferred_element_type=F32)
        partial = lax.dot_general(hidden, weight, across, preferred_element_type=F32)
        out[:, place * 256 : (place + 1) * 256] = (partial * scale[0:1, :]).astype(BF16)


def gathered_kernel(own, plus, across, minus, first, second):
    x = lax.axis_index("x")
    for offset, ref in enumerate((own, plus, across, minus)):
        place = lax.rem(x + offset, 4)

        @pl.when(place < 2)
        def _():
            first[lax.rem(place, 2)] = ref[...]

        @pl.when(place >= 2)
        def _():
            second[lax.rem(place, 2)] = ref[...]


def finish_kernel(arrived, own_rows, out):
    zl, y = lax.axis_index("zl"), lax.axis_index("y")
    for place, k in enumerate((0, 1, -1, 2, -2, 3, -3, 4)):
        block = lax.rem(zl + k + 8, 8)
        columns = pl.ds(pl.multiple_of(block * 256, 256), 256)
        total = jnp.zeros((32, 256), F32)
        for i in range(8):
            total = total + arrived[i, :, place * 256 : (place + 1) * 256].astype(F32)
        total = jnp.where(y % 2 == 1, pltpu.roll(total, 64, 1), total)
        total = jnp.where(y >= 2, pltpu.roll(total, 128, 1), total)
        out[:, columns] = (own_rows[:, columns] + total).astype(BF16)


def shards(
    stream, gain_mix, w_query, scale_query, w_key, scale_key, w_value, scale_value,
    gain_ffn, w_gate, scale_gate, w_up, scale_up, w_down, scale_down,
):
    hbm = pl.BlockSpec(memory_space=pltpu.HBM)
    qkv, ffn = call(
        pack_kernel,
        (jax.ShapeDtypeStruct((4, 64, 768), BF16), jax.ShapeDtypeStruct((96, 768), BF16)),
        *[
            pltpu.with_memory_space_constraint(array, pltpu.HBM)
            for array in (w_query, w_key, w_value, w_gate, w_up, w_down, scale_down[None])
        ],
        specs=[hbm] * 7,
        scratch=[pltpu.VMEM((64, n), F32) for n in (256, 256, 256, 352, 352, 352)]
        + [pltpu.VMEM((1, 64), F32), pltpu.SemaphoreType.DMA((7,))],
    )

    def rows_of(count):
        return jax.ShapeDtypeStruct((count, 768), BF16)

    fp1, fm1 = shift(ffn, Z, 1), shift(ffn, Z, -1)
    whole = lax.all_to_all(qkv, "y", split_axis=0, concat_axis=0, tiled=True).reshape(256, 768)
    own, own_m = call(first_kernel, (rows_of(352), rows_of(352)), whole, fp1, fm1)
    p1, m1 = shift(own, Z, 1), shift(own_m, Z, -1)
    p2, m2 = shift(p1, Z, 1), shift(m1, Z, -1)
    a0 = call(batch_a_kernel, rows_of(480), ffn, fp1, fm1, p1, m1)
    ap, am = shift(a0, "y", 1), shift(a0, "y", -1)
    p3, m3 = shift(p2[0:304], Z, 1), shift(m2[0:304], Z, -1)
    p4, m4 = shift(p3[0:128], Z, 1), shift(m3[128:256], Z, -1)
    b0, b0_m = call(batch_b_kernel, (rows_of(528), rows_of(528)), p2, m2, p3, m3, ap, am)
    bp, bm = shift(b0, "y", 1), shift(b0_m, "y", -1)
    b2p, b2m = shift(bp[0:144], "y", 1), shift(bm[144:288], "y", -1)

    stream_f = stream.astype(F32)
    square = jnp.mean(stream_f * stream_f, axis=-1, keepdims=True)
    normed = (stream_f * lax.rsqrt(square + EPS) * gain_mix).astype(BF16)
    angle = np.arange(LEN)[:, None] * THETA ** (-(np.arange(128) / 128))
    cosine, sine = jnp.asarray(np.cos(angle), F32), jnp.asarray(np.sin(angle), F32)
    decays = jnp.asarray(np.log(1.0 - 2.0 ** (-5.0 - np.arange(8))), F32)
    mixed = call(
        retention_kernel,
        jax.ShapeDtypeStruct((256, 256), BF16),
        decays, normed, own, p1, m1, p2, m2, p3, m3, p4, m4,
        scale_query[None], scale_key[None], scale_value[None], cosine, sine,
        specs=[SMEM] + [VMEM] * 15,
    )
    heads = [mixed] + [shift(mixed, "x", i) for i in (1, 2, 3)]
    pair = jax.ShapeDtypeStruct((2, 256, 256), BF16)
    first, second = call(gathered_kernel, (pair, pair), *heads)
    first, second = lax.all_gather(first, "c"), lax.all_gather(second, "c")
    wide = lambda scale: jnp.pad(scale, (0, 32))[None]
    partial, own_rows = call(
        ffn_kernel,
        (jax.ShapeDtypeStruct((256, 2048), BF16), jax.ShapeDtypeStruct((32, 2048), F32)),
        stream, first, second, gain_ffn.reshape(8, 1, 256),
        a0, ap, am, b0, bp, bm, b2p, b2m, wide(scale_gate), wide(scale_up),
        scratch=[pltpu.VMEM((8, 256, 256), F32)],
        limit=12,
    )
    arrived = lax.all_to_all(partial.reshape(8, 32, 2048), TP, split_axis=0, concat_axis=0, tiled=True)
    return call(
        finish_kernel, jax.ShapeDtypeStruct((32, 2048), BF16), arrived, own_rows
    )


def solution(mesh):
    torus = Mesh(
        mesh.devices.reshape(mesh.shape["rep"], mesh.shape["fs"] // 4, 4, 4, 2),
        ("zh", "zl", "y", "x", "c"),
    )
    rows, weight, columns = P(("zh", "zl", "y"), None), P(("zl", "y"), TP), P(TP)
    in_specs = (
        rows, P(), weight, columns, weight, columns, weight, columns,
        P(), weight, columns, weight, columns, weight, P(("zl", "y")),
    )
    return jax.shard_map(
        shards, mesh=torus, in_specs=in_specs, out_specs=P(("zh", "zl", "y", "x", "c"), None), check_vma=False
    )
```

```python
import jax
import jax.numpy as jnp
import numpy as np
from jax import lax
from jax.experimental import pallas as pl
from jax.experimental.pallas import tpu as pltpu
from jax.sharding import Mesh
from jax.sharding import PartitionSpec as P


EPS = 1e-06
THETA = 10000.0
HIGH = lax.Precision.HIGHEST
LEN = 128
Z = ("zh", "zl")
TP = ("x", "c")
F32 = jnp.float32
BF16 = jnp.bfloat16
VMEM = pl.BlockSpec(memory_space=pltpu.VMEM)
MIB = 1 << 20


def shift(array, axis, offset):
    n = lax.axis_size(axis)
    return lax.ppermute(array, axis, [((i + offset) % n, i) for i in range(n)])


def call(kernel, out_shape, *args, scratch=(), specs=None, limit=6):
    return pl.pallas_call(
        kernel,
        out_shape=out_shape,
        in_specs=specs or [VMEM] * len(args),
        out_specs=jax.tree.map(lambda _: VMEM, out_shape),
        scratch_shapes=list(scratch),
        compiler_params=pltpu.CompilerParams(vmem_limit_bytes=limit * MIB),
    )(*args)


def pack_kernel(*refs):
    sources, qkv, ffn, held, sems = refs[:7], refs[7], refs[8], refs[9:16], refs[16]
    copies = [pltpu.make_async_copy(sources[i], held[i], sems.at[i]) for i in range(7)]
    for copy in copies:
        copy.start()
    copies[6].wait()
    diagonal = lax.broadcasted_iota(jnp.int32, (64, 64), 0) == lax.broadcasted_iota(jnp.int32, (64, 64), 1)
    scale = jnp.sum(jnp.where(diagonal, held[6][...], 0.0), axis=1, keepdims=True)
    high = scale.astype(BF16).astype(F32)
    middle = (scale - high).astype(BF16).astype(F32)
    low = scale - high - middle
    lane = lax.broadcasted_iota(jnp.int32, (64, 384), 1)
    extra = jnp.where(lane == 352, high, jnp.where(lane == 353, middle, jnp.where(lane == 354, low, 0.0)))
    extra = extra.astype(BF16)
    ffn[0:64, :] = jnp.zeros((64, 768), BF16)
    ffn[64:96, 0:384] = extra[0:32]
    ffn[64:96, 384:768] = extra[32:64]
    for copy in copies[:6]:
        copy.wait()
    wq, wk, wv, wg, wu, wd = held[:6]
    for copy in range(4):
        qkv[copy, :, 0:256] = wq[...].astype(BF16)
        qkv[copy, :, 256:512] = wk[...].astype(BF16)
        qkv[copy, :, 512:768] = wv[...].astype(BF16)
    ffn[0:64, 0:352] = wg[...].astype(BF16)
    ffn[0:64, 384:736] = wu[...].astype(BF16)
    down = wd[...].astype(BF16)
    ffn[64:96, 0:352] = down[0:32]
    ffn[64:96, 384:736] = down[32:64]


def first_plus_kernel(qkv, ffn, out):
    out[0:256, :] = qkv[...]
    out[256:352, :] = ffn[...]


def first_minus_kernel(qkv, ffn, out):
    out[0:256, :] = qkv[...]
    out[256:304, :] = ffn[48:96, :]
    out[304:352, :] = ffn[0:48, :]


def near_rows(out, start, plus, minus):
    out[start : start + 96, :] = plus[256:352, :]
    out[start + 96 : start + 144, :] = minus[304:352, :]
    out[start + 144 : start + 192, :] = minus[256:304, :]


def round_a_kernel(own, fp1, fm1, p1, m1, out):
    out[0:96, :] = own[...]
    out[96:192, :] = fp1[...]
    out[192:288, :] = fm1[...]
    near_rows(out, 288, p1, m1)


def round_b_kernel(p2, m2, out):
    near_rows(out, 0, p2, m2)


def round_c_kernel(p3, m3, bp, bm, ap, am, plus, minus, own):
    for out in (plus, minus, own):
        out[0:48, :] = p3[256:304, :]
        out[48:96, :] = m3[256:304, :]
    plus[96:192, :] = bp[0:96, :]
    minus[96:192, :] = bm[96:192, :]
    plus[192:432, :] = ap[0:240, :]
    minus[192:432, :] = am[240:480, :]


def early_kernel(
    stream, gain_mix, cosine, sine, sq, sk, sv, sg, su, gain_ffn, normed, tables, scales, wide, gain
):
    rows = stream[...].astype(F32)
    square = jnp.mean(rows * rows, axis=-1, keepdims=True)
    normed[...] = (rows * lax.rsqrt(square + EPS) * gain_mix[...]).astype(BF16)
    tables[0] = cosine[...]
    tables[1] = sine[...]
    for i, ref in enumerate((sq, sk, sv)):
        scales[i] = ref[...]
    for i, ref in enumerate((sg, su)):
        wide[i] = jnp.zeros((1, 384), F32)
        wide[i, :, 0:352] = ref[...]
    gain[...] = gain_ffn[...]


def retention_kernel(normed, own, p1, m1, p2, m2, p3, m3, p4, scales, tables, out):
    zl = lax.axis_index("zl")
    head, decay = lax.axis_index(TP), jnp.float32(0.0)
    for h in range(8):
        decay = jnp.where(head == h, jnp.float32(np.log(1.0 - 2.0 ** (-5 - h))), decay)
    acc = jnp.zeros((256, 768), F32)
    blocks = {0: own, 1: p1, -1: m1, 2: p2, -2: m2, 3: p3, -3: m3}
    for k in (0, 1, -1, 2, -2, 3, -3, 4):
        block = lax.rem(zl + k + 8, 8)
        rows = normed[:, pl.ds(pl.multiple_of(block * 256, 256), 256)]
        weight = p4[...] if k == 4 else blocks[k][0:256, :]
        acc = acc + jnp.dot(rows, weight, preferred_element_type=F32)
    query = (acc[:, 0:256] * scales[0]).astype(BF16).astype(F32)
    key = (acc[:, 256:512] * scales[1]).astype(BF16).astype(F32)
    value = (acc[:, 512:768] * scales[2]).astype(BF16).astype(F32)
    cos = tables[0]
    sin = tables[1]
    distance = lax.broadcasted_iota(jnp.int32, (LEN, LEN), 0) - lax.broadcasted_iota(jnp.int32, (LEN, LEN), 1)
    distance = distance.astype(F32)
    mask = jnp.where(distance >= 0, jnp.exp(decay * jnp.maximum(distance, 0.0)), 0.0)

    def rotate(values):
        first, second = values[:, 0:128], values[:, 128:256]
        return jnp.concatenate([first * cos - second * sin, second * cos + first * sin], axis=1)

    for s in range(2):
        rows = slice(s * LEN, (s + 1) * LEN)
        rot_query = rotate(query[rows])
        rot_key = rotate(key[rows]) * (256**-0.5)
        scores = lax.dot_general(
            rot_query, rot_key, (((1,), (1,)), ((), ())), precision=HIGH, preferred_element_type=F32
        )
        retained = jnp.dot(scores * mask, value[rows], precision=HIGH, preferred_element_type=F32)
        square = jnp.mean(retained * retained, axis=-1, keepdims=True)
        mixed = (retained * (1.0 / jnp.maximum(jnp.sqrt(square), 1.0))).astype(BF16)
        out[rows, :] = mixed


def ffn_kernel(
    stream, heads, others, gain, a0, ap, am, b0, bp, bm, c0, cp, cm, d2, wide,
    keep, send, own_rows, resid,
):
    zl, y, tp = lax.axis_index("zl"), lax.axis_index("y"), lax.axis_index(TP)
    odd = lax.axis_index("c") == 1
    total = jnp.zeros((256, 1), F32)
    for b in range(8):
        head = jnp.where(odd == (b % 2 == 1), heads[b // 2].astype(F32), others[b // 2].astype(F32))
        rows = stream[:, b * 256 : (b + 1) * 256].astype(F32) + head
        resid[b] = rows
        total = total + jnp.sum(rows * rows, axis=-1, keepdims=True)
        own_rows[:, b * 256 : (b + 1) * 256] = resid[b, pl.ds(pl.multiple_of(tp * 32, 32), 32), :]
    inverse = lax.rsqrt(total * (1.0 / 2048) + EPS)
    mine = {
        0: [(a0, 0, 96)], 1: [(a0, 96, 96)], -1: [(a0, 192, 96)], 2: [(a0, 288, 96)], -2: [(a0, 384, 96)],
        3: [(b0, 0, 96)], -3: [(b0, 96, 96)], 4: [(c0, 0, 96)],
    }
    across = {
        0: [(cp, 192, 96)], 1: [(cp, 288, 96)], -1: [(cp, 384, 48), (cm, 192, 48)], 2: [(cm, 240, 96)],
        -2: [(cm, 336, 96)], 3: [(cp, 96, 96)], -3: [(cm, 96, 96)], 4: [(d2, 0, 96)],
    }
    plus = {id(a0): ap, id(b0): bp, id(c0): cp}
    minus = {id(a0): am, id(b0): bm, id(c0): cm}

    def shard(k, j, start, stop):
        pieces, base = [], 0
        for ref, low, count in across[k] if j == 2 else mine[k]:
            ref = plus[id(ref)] if j == 1 else minus[id(ref)] if j == 3 else ref
            begin, end = max(start, base), min(stop, base + count)
            if begin < end:
                pieces.append(ref[low + begin - base : low + end - base, :])
            base += count
        return pieces[0] if len(pieces) == 1 else jnp.concatenate(pieces, axis=0)

    def turned(values, by_one, by_two):
        values = jnp.where(by_one, pltpu.roll(values, 192, 1), values)
        return jnp.where(by_two, pltpu.roll(values, 128, 1), values)

    acc = jnp.zeros((256, 768), F32)
    order = (0, 1, -1, 2, -2, 3, -3, 4)
    for k in order:
        block = lax.rem(zl + k + 8, 8)
        rows = turned(resid[block] * inverse * gain[block], y % 2 == 1, y >= 2).astype(BF16)
        weight = jnp.concatenate([shard(k, j, 0, 64) for j in range(4)], axis=0)
        acc = acc + jnp.dot(rows, weight, preferred_element_type=F32)
    gate = acc[:, 0:384] * wide[0]
    hidden = (gate / (1.0 + jnp.exp(-gate)) * (acc[:, 384:768] * wide[1])).astype(BF16)
    lane = lax.broadcasted_iota(jnp.int32, (16, 384), 1)
    pick = jnp.where((lane >= 352) & (lane <= 354), 1.0, 0.0).astype(BF16)
    for place, k in enumerate(order):
        pieces = []
        for j in range(4):
            piece = shard(k, j, 64, 96)
            pieces += [piece[:, 0:384], piece[:, 384:768]]
        weight = jnp.concatenate(pieces, axis=0)
        both = (((1,), (1,)), ((), ()))
        scale = lax.dot_general(pick, weight, both, preferred_element_type=F32)
        partial = lax.dot_general(hidden, weight, both, preferred_element_type=F32) * scale[0:1, :]
        partial = partial.reshape(4, 2, 32, 256)
        north, south = partial[:, 1].reshape(128, 256), partial[:, 0].reshape(128, 256)
        columns = slice(place * 256, (place + 1) * 256)
        send[:, columns] = jnp.where(odd, south, north).astype(BF16)
        keep[:, columns] = jnp.where(odd, north, south)


def pair_kernel(keep, other, out):
    for i in range(4):
        rows = slice(i * 32, (i + 1) * 32)
        out[i] = (keep[rows, :] + other[rows, :].astype(F32)).astype(BF16)


def finish_kernel(arrived, own_rows, out):
    zl, y = lax.axis_index("zl"), lax.axis_index("y")
    for place, k in enumerate((0, 1, -1, 2, -2, 3, -3, 4)):
        block = lax.rem(zl + k + 8, 8)
        columns = pl.ds(pl.multiple_of(block * 256, 256), 256)
        total = jnp.zeros((32, 256), F32)
        for i in range(4):
            total = total + arrived[i, :, place * 256 : (place + 1) * 256].astype(F32)
        total = jnp.where(y % 2 == 1, pltpu.roll(total, 64, 1), total)
        total = jnp.where(y >= 2, pltpu.roll(total, 128, 1), total)
        out[:, columns] = (own_rows[:, columns] + total).astype(BF16)


def shards(
    stream, gain_mix, w_query, scale_query, w_key, scale_key, w_value, scale_value,
    gain_ffn, w_gate, scale_gate, w_up, scale_up, w_down, scale_down,
):
    hbm = pl.BlockSpec(memory_space=pltpu.HBM)
    qkv, ffn = call(
        pack_kernel,
        (jax.ShapeDtypeStruct((4, 64, 768), BF16), jax.ShapeDtypeStruct((96, 768), BF16)),
        *[
            pltpu.with_memory_space_constraint(array, pltpu.HBM)
            for array in (w_query, w_key, w_value, w_gate, w_up, w_down, scale_down[None])
        ],
        specs=[hbm] * 7,
        scratch=[pltpu.VMEM((64, n), F32) for n in (256, 256, 256, 352, 352, 352)]
        + [pltpu.VMEM((1, 64), F32), pltpu.SemaphoreType.DMA((7,))],
    )

    def rows_of(count):
        return jax.ShapeDtypeStruct((count, 768), BF16)

    fp1, fm1 = shift(ffn, Z, 1), shift(ffn, Z, -1)
    whole = lax.all_to_all(qkv, "y", split_axis=0, concat_axis=0, tiled=True).reshape(256, 768)
    own = call(first_plus_kernel, rows_of(352), whole, fp1)
    own_m = call(first_minus_kernel, rows_of(352), whole, fm1)
    p1, m1 = shift(own, Z, 1), shift(own_m, Z, -1)
    p2, m2 = shift(p1, Z, 1), shift(m1, Z, -1)
    angle = np.arange(LEN)[:, None] * THETA ** (-(np.arange(128) / 128))
    normed, tables, scales, wide, gain = call(
        early_kernel,
        tuple(
            jax.ShapeDtypeStruct(shape, kind)
            for shape, kind in (
                ((256, 2048), BF16), ((2, LEN, 128), F32), ((3, 1, 256), F32), ((2, 1, 384), F32), ((8, 1, 256), F32)
            )
        ),
        stream, gain_mix[None], jnp.asarray(np.cos(angle), F32), jnp.asarray(np.sin(angle), F32),
        scale_query[None], scale_key[None], scale_value[None], scale_gate[None], scale_up[None],
        gain_ffn.reshape(8, 1, 256), limit=12,
    )
    a0 = call(round_a_kernel, rows_of(480), ffn, fp1, fm1, p1, m1)
    ap, am = shift(a0, "y", 1), shift(a0, "y", -1)
    p3, m3 = shift(p2[0:304], Z, 1), shift(m2[0:304], Z, -1)
    b0 = call(round_b_kernel, rows_of(192), p2, m2)
    bp, bm = shift(b0, "y", 1), shift(b0, "y", -1)
    p4 = shift(p3[0:256], Z, 1)
    c0, c0_m, last = call(round_c_kernel, (rows_of(432), rows_of(432), rows_of(96)), p3, m3, bp, bm, ap, am)
    cp, cm = shift(c0, "y", 1), shift(c0_m, "y", -1)
    d2 = shift(last, "y", 2)

    mixed = call(
        retention_kernel,
        jax.ShapeDtypeStruct((256, 256), BF16),
        normed, own, p1, m1, p2, m2, p3, m3, p4, scales, tables,
    )
    heads = lax.all_gather(mixed, "x")
    others = shift(heads, "c", 1)
    keep, send, own_rows = call(
        ffn_kernel,
        (
            jax.ShapeDtypeStruct((128, 2048), F32),
            jax.ShapeDtypeStruct((128, 2048), BF16),
            jax.ShapeDtypeStruct((32, 2048), F32),
        ),
        stream, heads, others, gain, a0, ap, am, b0, bp, bm, c0, cp, cm, d2, wide,
        scratch=[pltpu.VMEM((8, 256, 256), F32)],
        limit=12,
    )
    partial = call(pair_kernel, jax.ShapeDtypeStruct((4, 32, 2048), BF16), keep, shift(send, "c", 1))
    arrived = lax.all_to_all(partial, "x", split_axis=0, concat_axis=0, tiled=True)
    return call(
        finish_kernel, jax.ShapeDtypeStruct((32, 2048), BF16), arrived, own_rows
    )


def solution(mesh):
    torus = Mesh(
        mesh.devices.reshape(mesh.shape["rep"], mesh.shape["fs"] // 4, 4, 4, 2),
        ("zh", "zl", "y", "x", "c"),
    )
    rows, weight, columns = P(("zh", "zl", "y"), None), P(("zl", "y"), TP), P(TP)
    in_specs = (
        rows, P(), weight, columns, weight, columns, weight, columns,
        P(), weight, columns, weight, columns, weight, P(("zl", "y")),
    )
    return jax.shard_map(
        shards, mesh=torus, in_specs=in_specs, out_specs=P(("zh", "zl", "y", "x", "c"), None), check_vma=False
    )
```

```python
import jax
import jax.numpy as jnp
import numpy as np
from jax import lax
from jax.experimental import pallas as pl
from jax.experimental.pallas import tpu as pltpu
from jax.sharding import Mesh
from jax.sharding import PartitionSpec as P


EPS = 1e-06
THETA = 10000.0
HIGH = lax.Precision.HIGHEST
LEN = 128
Z = ("zh", "zl")
TP = ("x", "c")
F32 = jnp.float32
BF16 = jnp.bfloat16
VMEM = pl.BlockSpec(memory_space=pltpu.VMEM)
MIB = 1 << 20


def shift(array, axis, offset):
    n = lax.axis_size(axis)
    return lax.ppermute(array, axis, [((i + offset) % n, i) for i in range(n)])


def call(kernel, out_shape, *args, scratch=(), specs=None, limit=6):
    return pl.pallas_call(
        kernel,
        out_shape=out_shape,
        in_specs=specs or [VMEM] * len(args),
        out_specs=jax.tree.map(lambda _: VMEM, out_shape),
        scratch_shapes=list(scratch),
        compiler_params=pltpu.CompilerParams(vmem_limit_bytes=limit * MIB),
    )(*args)


def pack_kernel(*refs):
    sources, qkv, ffn, held, sems = refs[:7], refs[7], refs[8], refs[9:16], refs[16]
    copies = [pltpu.make_async_copy(sources[i], held[i], sems.at[i]) for i in range(7)]
    for copy in copies:
        copy.start()
    copies[6].wait()
    diagonal = lax.broadcasted_iota(jnp.int32, (64, 64), 0) == lax.broadcasted_iota(jnp.int32, (64, 64), 1)
    scale = jnp.sum(jnp.where(diagonal, held[6][...], 0.0), axis=1, keepdims=True)
    high = scale.astype(BF16).astype(F32)
    middle = (scale - high).astype(BF16).astype(F32)
    low = scale - high - middle
    lane = lax.broadcasted_iota(jnp.int32, (64, 384), 1)
    extra = jnp.where(lane == 352, high, jnp.where(lane == 353, middle, jnp.where(lane == 354, low, 0.0)))
    extra = extra.astype(BF16)
    ffn[0:64, :] = jnp.zeros((64, 768), BF16)
    ffn[64:96, 0:384] = extra[0:32]
    ffn[64:96, 384:768] = extra[32:64]
    for copy in copies[:6]:
        copy.wait()
    wq, wk, wv, wg, wu, wd = held[:6]
    for copy in range(4):
        qkv[copy, :, 0:256] = wq[...].astype(BF16)
        qkv[copy, :, 256:512] = wk[...].astype(BF16)
        qkv[copy, :, 512:768] = wv[...].astype(BF16)
    ffn[0:64, 0:352] = wg[...].astype(BF16)
    ffn[0:64, 384:736] = wu[...].astype(BF16)
    down = wd[...].astype(BF16)
    ffn[64:96, 0:352] = down[0:32]
    ffn[64:96, 384:736] = down[32:64]


def first_plus_kernel(qkv, ffn, out):
    out[0:256, :] = qkv[...]
    out[256:352, :] = ffn[...]


def first_minus_kernel(qkv, ffn, out):
    out[0:256, :] = qkv[...]
    out[256:304, :] = ffn[48:96, :]
    out[304:352, :] = ffn[0:48, :]


def near_rows(out, start, plus, minus):
    out[start : start + 96, :] = plus[256:352, :]
    out[start + 96 : start + 144, :] = minus[304:352, :]
    out[start + 144 : start + 192, :] = minus[256:304, :]


def round_a_kernel(own, fp1, fm1, p1, m1, out):
    out[0:96, :] = own[...]
    out[96:192, :] = fp1[...]
    out[192:288, :] = fm1[...]
    near_rows(out, 288, p1, m1)


def round_b_kernel(p2, m2, out):
    near_rows(out, 0, p2, m2)


def round_c_kernel(p3, m3, bp, bm, ap, am, plus, minus, own):
    for out in (plus, minus, own):
        out[0:48, :] = p3[256:304, :]
        out[48:96, :] = m3[256:304, :]
    plus[96:192, :] = bp[0:96, :]
    minus[96:192, :] = bm[96:192, :]
    plus[192:432, :] = ap[0:240, :]
    minus[192:432, :] = am[240:480, :]


def early_kernel(
    stream, gain_mix, cosine, sine, sq, sk, sv, sg, su, gain_ffn, normed, tables, scales, wide, gain
):
    rows = stream[...].astype(F32)
    square = jnp.mean(rows * rows, axis=-1, keepdims=True)
    normed[...] = (rows * lax.rsqrt(square + EPS) * gain_mix[...]).astype(BF16)
    tables[0] = cosine[...]
    tables[1] = sine[...]
    for i, ref in enumerate((sq, sk, sv)):
        scales[i] = ref[...]
    for i, ref in enumerate((sg, su)):
        wide[i] = jnp.zeros((1, 384), F32)
        wide[i, :, 0:352] = ref[...]
    gain[...] = gain_ffn[...]


def retention_kernel(normed, own, p1, m1, p2, m2, p3, m3, p4, scales, tables, out):
    zl = lax.axis_index("zl")
    head, decay = lax.axis_index(TP), jnp.float32(0.0)
    for h in range(8):
        decay = jnp.where(head == h, jnp.float32(np.log(1.0 - 2.0 ** (-5 - h))), decay)
    acc = jnp.zeros((256, 768), F32)
    blocks = {0: own, 1: p1, -1: m1, 2: p2, -2: m2, 3: p3, -3: m3}
    for k in (0, 1, -1, 2, -2, 3, -3, 4):
        block = lax.rem(zl + k + 8, 8)
        rows = normed[:, pl.ds(pl.multiple_of(block * 256, 256), 256)]
        weight = p4[...] if k == 4 else blocks[k][0:256, :]
        acc = acc + jnp.dot(rows, weight, preferred_element_type=F32)
    query = (acc[:, 0:256] * scales[0]).astype(BF16).astype(F32)
    key = (acc[:, 256:512] * scales[1]).astype(BF16).astype(F32)
    value = (acc[:, 512:768] * scales[2]).astype(BF16).astype(F32)
    cos = tables[0]
    sin = tables[1]
    distance = lax.broadcasted_iota(jnp.int32, (LEN, LEN), 0) - lax.broadcasted_iota(jnp.int32, (LEN, LEN), 1)
    distance = distance.astype(F32)
    mask = jnp.where(distance >= 0, jnp.exp(decay * jnp.maximum(distance, 0.0)), 0.0)

    def rotate(values):
        first, second = values[:, 0:128], values[:, 128:256]
        return jnp.concatenate([first * cos - second * sin, second * cos + first * sin], axis=1)

    for s in range(2):
        rows = slice(s * LEN, (s + 1) * LEN)
        rot_query = rotate(query[rows])
        rot_key = rotate(key[rows]) * (256**-0.5)
        scores = lax.dot_general(
            rot_query, rot_key, (((1,), (1,)), ((), ())), precision=HIGH, preferred_element_type=F32
        )
        retained = jnp.dot(scores * mask, value[rows], precision=HIGH, preferred_element_type=F32)
        square = jnp.mean(retained * retained, axis=-1, keepdims=True)
        mixed = (retained * (1.0 / jnp.maximum(jnp.sqrt(square), 1.0))).astype(BF16)
        out[rows, :] = mixed


NAMES = ("a0", "ap", "am", "b0", "bp", "bm", "c0", "cp", "cm", "d2")
MINE = {
    0: [("a", 0, 96)], 1: [("a", 96, 96)], -1: [("a", 192, 96)], 2: [("a", 288, 96)], -2: [("a", 384, 96)],
    3: [("b", 0, 96)], -3: [("b", 96, 96)], 4: [("c", 0, 96)],
}
ACROSS = {
    0: [("cp", 192, 96)], 1: [("cp", 288, 96)], -1: [("cp", 384, 48), ("cm", 192, 48)], 2: [("cm", 240, 96)],
    -2: [("cm", 336, 96)], 3: [("cp", 96, 96)], -3: [("cm", 96, 96)], 4: [("d2", 0, 96)],
}


def shard(refs, k, j, start, stop):
    pieces, base = [], 0
    for name, low, count in ACROSS[k] if j == 2 else MINE[k]:
        ref = refs[name if j == 2 else name + {0: "0", 1: "p", 3: "m"}[j]]
        begin, end = max(start, base), min(stop, base + count)
        if begin < end:
            pieces.append(ref[low + begin - base : low + end - base, :])
        base += count
    return pieces[0] if len(pieces) == 1 else jnp.concatenate(pieces, axis=0)


def half_sums(refs, side, stream, heads, gain, resid, acc):
    zl, y = lax.axis_index("zl"), lax.axis_index("y")
    total = jnp.zeros((256, 1), F32)
    for i in range(4):
        columns = pl.ds(pl.multiple_of((2 * i + side) * 256, 256), 256)
        rows = stream[:, columns].astype(F32) + heads[i].astype(F32)
        resid[i] = rows
        total = total + jnp.sum(rows * rows, axis=-1, keepdims=True)

    def add(offsets):
        result = None
        for k in offsets:
            block = lax.rem(zl + k + 8, 8)
            rows = resid[lax.div(block, 2)] * gain[block]
            rows = jnp.where(y % 2 == 1, pltpu.roll(rows, 192, 1), rows)
            rows = jnp.where(y >= 2, pltpu.roll(rows, 128, 1), rows).astype(BF16)
            weight = jnp.concatenate([shard(refs, k, j, 0, 64) for j in range(4)], axis=0)
            part = jnp.dot(rows, weight, preferred_element_type=F32)
            result = part if result is None else result + part
        acc[...] = result

    even = lax.rem(zl + side, 2) == 0

    @pl.when(even)
    def _():
        add((0, 2, -2, 4))

    @pl.when(jnp.logical_not(even))
    def _():
        add((1, -1, 3, -3))

    return total


def ffn_own_kernel(stream, heads, gain, *rest):
    refs = dict(zip(NAMES, rest))
    resid, acc, total = rest[len(NAMES) :]
    total[...] = half_sums(refs, lax.axis_index("c"), stream, heads, gain, resid, acc)


def rows_for(hidden, side):
    hidden = hidden.reshape(4, 2, 32, hidden.shape[-1])
    both = [hidden[:, i].reshape(128, hidden.shape[-1]) for i in range(2)]
    return jnp.where(side == 1, both[1], both[0])


def down_sums(refs, hidden, out):
    lane = lax.broadcasted_iota(jnp.int32, (16, 384), 1)
    pick = jnp.where((lane >= 352) & (lane <= 354), 1.0, 0.0).astype(BF16)
    hidden = jnp.concatenate([hidden, pick], axis=0)
    for place, k in enumerate((0, 1, -1, 2, -2, 3, -3, 4)):
        pieces = []
        for j in range(4):
            piece = shard(refs, k, j, 64, 96)
            pieces += [piece[:, 0:384], piece[:, 384:768]]
        weight = jnp.concatenate(pieces, axis=0)
        sums = lax.dot_general(hidden, weight, (((1,), (1,)), ((), ())), preferred_element_type=F32)
        out[:, place * 256 : (place + 1) * 256] = (sums[0:128] * sums[128:129]).astype(out.dtype)


def ffn_kernel(stream, heads, gain, own_resid, own_acc, own_total, wide, *rest):
    refs = dict(zip(NAMES, rest))
    send, kept, own_rows, resid, acc = rest[len(NAMES) :]
    c, tp = lax.axis_index("c"), lax.axis_index(TP)
    total = own_total[...] + half_sums(refs, 1 - c, stream, heads, gain, resid, acc)
    mine = pl.ds(pl.multiple_of(tp * 32, 32), 32)
    for i in range(4):
        for side, ref in ((c, own_resid), (1 - c, resid)):
            columns = pl.ds(pl.multiple_of((2 * i + side) * 256, 256), 256)
            own_rows[:, columns] = ref[i, mine, :]
    inverse = lax.rsqrt(total * (1.0 / 2048) + EPS)
    sums = (own_acc[...] + acc[...]) * inverse
    gate = sums[:, 0:384] * wide[0]
    hidden = gate / (1.0 + jnp.exp(-gate)) * (sums[:, 384:768] * wide[1])
    kept[...] = rows_for(hidden, c).astype(BF16)
    down_sums(refs, rows_for(hidden, 1 - c).astype(BF16), send)


def down_kernel(hidden, *rest):
    down_sums(dict(zip(NAMES, rest)), hidden[...], rest[len(NAMES)])


def pair_kernel(keep, other, out):
    for i in range(4):
        rows = slice(i * 32, (i + 1) * 32)
        out[i] = (keep[rows, :] + other[rows, :].astype(F32)).astype(BF16)


def finish_kernel(arrived, own_rows, out):
    zl, y = lax.axis_index("zl"), lax.axis_index("y")
    for place, k in enumerate((0, 1, -1, 2, -2, 3, -3, 4)):
        block = lax.rem(zl + k + 8, 8)
        columns = pl.ds(pl.multiple_of(block * 256, 256), 256)
        total = jnp.zeros((32, 256), F32)
        for i in range(4):
            total = total + arrived[i, :, place * 256 : (place + 1) * 256].astype(F32)
        total = jnp.where(y % 2 == 1, pltpu.roll(total, 64, 1), total)
        total = jnp.where(y >= 2, pltpu.roll(total, 128, 1), total)
        out[:, columns] = (own_rows[:, columns] + total).astype(BF16)


def shards(
    stream, gain_mix, w_query, scale_query, w_key, scale_key, w_value, scale_value,
    gain_ffn, w_gate, scale_gate, w_up, scale_up, w_down, scale_down,
):
    hbm = pl.BlockSpec(memory_space=pltpu.HBM)
    qkv, ffn = call(
        pack_kernel,
        (jax.ShapeDtypeStruct((4, 64, 768), BF16), jax.ShapeDtypeStruct((96, 768), BF16)),
        *[
            pltpu.with_memory_space_constraint(array, pltpu.HBM)
            for array in (w_query, w_key, w_value, w_gate, w_up, w_down, scale_down[None])
        ],
        specs=[hbm] * 7,
        scratch=[pltpu.VMEM((64, n), F32) for n in (256, 256, 256, 352, 352, 352)]
        + [pltpu.VMEM((1, 64), F32), pltpu.SemaphoreType.DMA((7,))],
    )

    def rows_of(count):
        return jax.ShapeDtypeStruct((count, 768), BF16)

    fp1, fm1 = shift(ffn, Z, 1), shift(ffn, Z, -1)
    whole = lax.all_to_all(qkv, "y", split_axis=0, concat_axis=0, tiled=True).reshape(256, 768)
    own = call(first_plus_kernel, rows_of(352), whole, fp1)
    own_m = call(first_minus_kernel, rows_of(352), whole, fm1)
    p1, m1 = shift(own, Z, 1), shift(own_m, Z, -1)
    p2, m2 = shift(p1, Z, 1), shift(m1, Z, -1)
    angle = np.arange(LEN)[:, None] * THETA ** (-(np.arange(128) / 128))
    normed, tables, scales, wide, gain = call(
        early_kernel,
        tuple(
            jax.ShapeDtypeStruct(shape, kind)
            for shape, kind in (
                ((256, 2048), BF16), ((2, LEN, 128), F32), ((3, 1, 256), F32), ((2, 1, 384), F32), ((8, 1, 256), F32)
            )
        ),
        stream, gain_mix[None], jnp.asarray(np.cos(angle), F32), jnp.asarray(np.sin(angle), F32),
        scale_query[None], scale_key[None], scale_value[None], scale_gate[None], scale_up[None],
        gain_ffn.reshape(8, 1, 256), limit=12,
    )
    a0 = call(round_a_kernel, rows_of(480), ffn, fp1, fm1, p1, m1)
    ap, am = shift(a0, "y", 1), shift(a0, "y", -1)
    p3, m3 = shift(p2[0:304], Z, 1), shift(m2[0:304], Z, -1)
    b0 = call(round_b_kernel, rows_of(192), p2, m2)
    bp, bm = shift(b0, "y", 1), shift(b0, "y", -1)
    p4 = shift(m3[0:256], Z, -1)
    c0, c0_m, last = call(round_c_kernel, (rows_of(432), rows_of(432), rows_of(96)), p3, m3, bp, bm, ap, am)
    cp, cm = shift(c0, "y", 1), shift(c0_m, "y", -1)
    d2 = shift(last, "y", 2)

    mixed = call(
        retention_kernel,
        jax.ShapeDtypeStruct((256, 256), BF16),
        normed, own, p1, m1, p2, m2, p3, m3, p4, scales, tables,
    )
    heads = lax.all_gather(mixed, "x", axis=0)
    others = shift(heads, "c", 1)
    shards_of_ffn = (a0, ap, am, b0, bp, bm, c0, cp, cm, d2)
    own_resid, own_acc, own_total = call(
        ffn_own_kernel,
        tuple(jax.ShapeDtypeStruct(shape, F32) for shape in ((4, 256, 256), (256, 768), (256, 1))),
        stream, heads, gain, *shards_of_ffn, limit=12,
    )
    send, kept, own_rows = call(
        ffn_kernel,
        (
            jax.ShapeDtypeStruct((128, 2048), BF16),
            jax.ShapeDtypeStruct((128, 384), BF16),
            jax.ShapeDtypeStruct((32, 2048), F32),
        ),
        stream, others, gain, own_resid, own_acc, own_total, wide, *shards_of_ffn,
        scratch=[pltpu.VMEM((4, 256, 256), F32), pltpu.VMEM((256, 768), F32)],
        limit=12,
    )
    other = shift(send, "c", 1)
    keep = call(down_kernel, jax.ShapeDtypeStruct((128, 2048), F32), kept, *shards_of_ffn, limit=12)
    partial = call(pair_kernel, jax.ShapeDtypeStruct((4, 32, 2048), BF16), keep, other)
    arrived = lax.all_to_all(partial, "x", split_axis=0, concat_axis=0, tiled=True)
    return call(
        finish_kernel, jax.ShapeDtypeStruct((32, 2048), BF16), arrived, own_rows
    )


def solution(mesh):
    torus = Mesh(
        mesh.devices.reshape(mesh.shape["rep"], mesh.shape["fs"] // 4, 4, 4, 2),
        ("zh", "zl", "y", "x", "c"),
    )
    rows, weight, columns = P(("zh", "zl", "y"), None), P(("zl", "y"), TP), P(TP)
    in_specs = (
        rows, P(), weight, columns, weight, columns, weight, columns,
        P(), weight, columns, weight, columns, weight, P(("zl", "y")),
    )
    return jax.shard_map(
        shards, mesh=torus, in_specs=in_specs, out_specs=P(("zh", "zl", "y", "x", "c"), None), check_vma=False
    )
```

```python
import jax
import jax.numpy as jnp
import numpy as np
from jax import lax
from jax.experimental import pallas as pl
from jax.experimental.pallas import tpu as pltpu
from jax.sharding import Mesh
from jax.sharding import PartitionSpec as P


EPS = 1e-06
THETA = 10000.0
HIGH = lax.Precision.HIGHEST
LEN = 128
Z = ("zh", "zl")
TP = ("x", "c")
F32 = jnp.float32
BF16 = jnp.bfloat16
VMEM = pl.BlockSpec(memory_space=pltpu.VMEM)
MIB = 1 << 20


def shift(array, axis, offset):
    n = lax.axis_size(axis)
    return lax.ppermute(array, axis, [((i + offset) % n, i) for i in range(n)])


def call(kernel, out_shape, *args, scratch=(), specs=None, limit=6):
    return pl.pallas_call(
        kernel,
        out_shape=out_shape,
        in_specs=specs or [VMEM] * len(args),
        out_specs=jax.tree.map(lambda _: VMEM, out_shape),
        scratch_shapes=list(scratch),
        compiler_params=pltpu.CompilerParams(vmem_limit_bytes=limit * MIB),
    )(*args)


def pack_kernel(*refs):
    sources, qkv, ffn, held, sems = refs[:7], refs[7], refs[8], refs[9:16], refs[16]
    copies = [pltpu.make_async_copy(sources[i], held[i], sems.at[i]) for i in range(7)]
    for copy in copies:
        copy.start()
    copies[6].wait()
    diagonal = lax.broadcasted_iota(jnp.int32, (64, 64), 0) == lax.broadcasted_iota(jnp.int32, (64, 64), 1)
    scale = jnp.sum(jnp.where(diagonal, held[6][...], 0.0), axis=1, keepdims=True)
    high = scale.astype(BF16).astype(F32)
    middle = (scale - high).astype(BF16).astype(F32)
    low = scale - high - middle
    lane = lax.broadcasted_iota(jnp.int32, (64, 384), 1)
    extra = jnp.where(lane == 352, high, jnp.where(lane == 353, middle, jnp.where(lane == 354, low, 0.0)))
    extra = extra.astype(BF16)
    ffn[0:64, :] = jnp.zeros((64, 768), BF16)
    ffn[64:96, 0:384] = extra[0:32]
    ffn[64:96, 384:768] = extra[32:64]
    for copy in copies[:6]:
        copy.wait()
    wq, wk, wv, wg, wu, wd = held[:6]
    for copy in range(4):
        qkv[copy, :, 0:256] = wq[...].astype(BF16)
        qkv[copy, :, 256:512] = wk[...].astype(BF16)
        qkv[copy, :, 512:768] = wv[...].astype(BF16)
    ffn[0:64, 0:352] = wg[...].astype(BF16)
    ffn[0:64, 384:736] = wu[...].astype(BF16)
    down = wd[...].astype(BF16)
    ffn[64:96, 0:352] = down[0:32]
    ffn[64:96, 384:736] = down[32:64]


def first_plus_kernel(qkv, ffn, out):
    out[0:256, :] = qkv[...]
    out[256:352, :] = ffn[...]


def first_minus_kernel(qkv, ffn, out):
    out[0:256, :] = qkv[...]
    out[256:304, :] = ffn[48:96, :]
    out[304:352, :] = ffn[0:48, :]


def near_rows(out, start, plus, minus):
    out[start : start + 96, :] = plus[256:352, :]
    out[start + 96 : start + 144, :] = minus[304:352, :]
    out[start + 144 : start + 192, :] = minus[256:304, :]


def round_a_kernel(own, fp1, fm1, p1, m1, out):
    out[0:96, :] = own[...]
    out[96:192, :] = fp1[...]
    out[192:288, :] = fm1[...]
    near_rows(out, 288, p1, m1)


def round_b_kernel(p2, m2, out):
    near_rows(out, 0, p2, m2)


def round_c_kernel(p3, m3, bp, bm, ap, am, plus, minus, own):
    for out in (plus, minus, own):
        out[0:48, :] = p3[256:304, :]
        out[48:96, :] = m3[256:304, :]
    plus[96:192, :] = bp[0:96, :]
    minus[96:192, :] = bm[96:192, :]
    plus[192:432, :] = ap[0:240, :]
    minus[192:432, :] = am[240:480, :]


def early_kernel(
    stream, gain_mix, cosine, sine, sq, sk, sv, sg, su, gain_ffn, normed, tables, scales, wide, gain
):
    rows = stream[...].astype(F32)
    square = jnp.mean(rows * rows, axis=-1, keepdims=True)
    normed[...] = (rows * lax.rsqrt(square + EPS) * gain_mix[...]).astype(BF16)
    tables[0] = cosine[...]
    tables[1] = sine[...]
    for i, ref in enumerate((sq, sk, sv)):
        scales[i] = ref[...]
    for i, ref in enumerate((sg, su)):
        wide[i] = jnp.zeros((1, 384), F32)
        wide[i, :, 0:352] = ref[...]
    gain[...] = gain_ffn[...]


def retention_kernel(normed, own, p1, m1, p2, m2, p3, m3, p4, scales, tables, out):
    zl = lax.axis_index("zl")
    head, decay = lax.axis_index(TP), jnp.float32(0.0)
    for h in range(8):
        decay = jnp.where(head == h, jnp.float32(np.log(1.0 - 2.0 ** (-5 - h))), decay)
    acc = jnp.zeros((256, 768), F32)
    blocks = {0: own, 1: p1, -1: m1, 2: p2, -2: m2, 3: p3, -3: m3}
    for k in (0, 1, -1, 2, -2, 3, -3, 4):
        block = lax.rem(zl + k + 8, 8)
        rows = normed[:, pl.ds(pl.multiple_of(block * 256, 256), 256)]
        weight = p4[...] if k == 4 else blocks[k][0:256, :]
        acc = acc + jnp.dot(rows, weight, preferred_element_type=F32)
    query = (acc[:, 0:256] * scales[0]).astype(BF16).astype(F32)
    key = (acc[:, 256:512] * scales[1]).astype(BF16).astype(F32)
    value = (acc[:, 512:768] * scales[2]).astype(BF16).astype(F32)
    cos = tables[0]
    sin = tables[1]
    distance = lax.broadcasted_iota(jnp.int32, (LEN, LEN), 0) - lax.broadcasted_iota(jnp.int32, (LEN, LEN), 1)
    distance = distance.astype(F32)
    mask = jnp.where(distance >= 0, jnp.exp(decay * jnp.maximum(distance, 0.0)), 0.0)

    def rotate(values):
        first, second = values[:, 0:128], values[:, 128:256]
        return jnp.concatenate([first * cos - second * sin, second * cos + first * sin], axis=1)

    for s in range(2):
        rows = slice(s * LEN, (s + 1) * LEN)
        rot_query = rotate(query[rows])
        rot_key = rotate(key[rows]) * (256**-0.5)
        scores = lax.dot_general(
            rot_query, rot_key, (((1,), (1,)), ((), ())), precision=HIGH, preferred_element_type=F32
        )
        retained = jnp.dot(scores * mask, value[rows], precision=HIGH, preferred_element_type=F32)
        square = jnp.mean(retained * retained, axis=-1, keepdims=True)
        mixed = (retained * (1.0 / jnp.maximum(jnp.sqrt(square), 1.0))).astype(BF16)
        for copy in range(4):
            out[copy, rows, :] = mixed


NAMES = ("a0", "ap", "am", "b0", "bp", "bm", "c0", "cp", "cm", "d2")
MINE = {
    0: [("a", 0, 96)], 1: [("a", 96, 96)], -1: [("a", 192, 96)], 2: [("a", 288, 96)], -2: [("a", 384, 96)],
    3: [("b", 0, 96)], -3: [("b", 96, 96)], 4: [("c", 0, 96)],
}
ACROSS = {
    0: [("cp", 192, 96)], 1: [("cp", 288, 96)], -1: [("cp", 384, 48), ("cm", 192, 48)], 2: [("cm", 240, 96)],
    -2: [("cm", 336, 96)], 3: [("cp", 96, 96)], -3: [("cm", 96, 96)], 4: [("d2", 0, 96)],
}


def shard(refs, k, j, start, stop):
    pieces, base = [], 0
    for name, low, count in ACROSS[k] if j == 2 else MINE[k]:
        ref = refs[name if j == 2 else name + {0: "0", 1: "p", 3: "m"}[j]]
        begin, end = max(start, base), min(stop, base + count)
        if begin < end:
            pieces.append(ref[low + begin - base : low + end - base, :])
        base += count
    return pieces[0] if len(pieces) == 1 else jnp.concatenate(pieces, axis=0)


def half_sums(refs, side, stream, heads, gain, resid, acc):
    zl, y = lax.axis_index("zl"), lax.axis_index("y")
    total = jnp.zeros((256, 1), F32)
    for i in range(4):
        columns = pl.ds(pl.multiple_of((2 * i + side) * 256, 256), 256)
        rows = stream[:, columns].astype(F32) + heads[i].astype(F32)
        resid[i] = rows
        total = total + jnp.sum(rows * rows, axis=-1, keepdims=True)

    def add(offsets):
        result = None
        for k in offsets:
            block = lax.rem(zl + k + 8, 8)
            rows = resid[lax.div(block, 2)] * gain[block]
            rows = jnp.where(y % 2 == 1, pltpu.roll(rows, 192, 1), rows)
            rows = jnp.where(y >= 2, pltpu.roll(rows, 128, 1), rows).astype(BF16)
            weight = jnp.concatenate([shard(refs, k, j, 0, 64) for j in range(4)], axis=0)
            part = jnp.dot(rows, weight, preferred_element_type=F32)
            result = part if result is None else result + part
        acc[...] = result

    even = lax.rem(zl + side, 2) == 0

    @pl.when(even)
    def _():
        add((0, 2, -2, 4))

    @pl.when(jnp.logical_not(even))
    def _():
        add((1, -1, 3, -3))

    return total


def ffn_own_kernel(stream, heads, gain, *rest):
    refs = dict(zip(NAMES, rest))
    resid, acc, total = rest[len(NAMES) :]
    total[...] = half_sums(refs, lax.axis_index("c"), stream, heads, gain, resid, acc)


def rows_for(hidden, side):
    hidden = hidden.reshape(4, 2, 32, hidden.shape[-1])
    both = [hidden[:, i].reshape(128, hidden.shape[-1]) for i in range(2)]
    return jnp.where(side == 1, both[1], both[0])


def down_sums(refs, hidden, out):
    lane = lax.broadcasted_iota(jnp.int32, (16, 384), 1)
    pick = jnp.where((lane >= 352) & (lane <= 354), 1.0, 0.0).astype(BF16)
    hidden = jnp.concatenate([hidden, pick], axis=0)
    for place, k in enumerate((0, 1, -1, 2, -2, 3, -3, 4)):
        pieces = []
        for j in range(4):
            piece = shard(refs, k, j, 64, 96)
            pieces += [piece[:, 0:384], piece[:, 384:768]]
        weight = jnp.concatenate(pieces, axis=0)
        sums = lax.dot_general(hidden, weight, (((1,), (1,)), ((), ())), preferred_element_type=F32)
        out[:, place * 256 : (place + 1) * 256] = (sums[0:128] * sums[128:129]).astype(out.dtype)


def ffn_kernel(stream, heads, gain, own_resid, own_acc, own_total, wide, *rest):
    refs = dict(zip(NAMES, rest))
    send, kept, own_rows, resid, acc = rest[len(NAMES) :]
    c, tp = lax.axis_index("c"), lax.axis_index(TP)
    total = own_total[...] + half_sums(refs, 1 - c, stream, heads, gain, resid, acc)
    mine = pl.ds(pl.multiple_of(tp * 32, 32), 32)
    for i in range(4):
        for side, ref in ((c, own_resid), (1 - c, resid)):
            columns = pl.ds(pl.multiple_of((2 * i + side) * 256, 256), 256)
            own_rows[:, columns] = ref[i, mine, :]
    inverse = lax.rsqrt(total * (1.0 / 2048) + EPS)
    sums = (own_acc[...] + acc[...]) * inverse
    gate = sums[:, 0:384] * wide[0]
    hidden = gate / (1.0 + jnp.exp(-gate)) * (sums[:, 384:768] * wide[1])
    kept[...] = rows_for(hidden, c).astype(BF16)
    down_sums(refs, rows_for(hidden, 1 - c).astype(BF16), send)


def down_kernel(hidden, *rest):
    down_sums(dict(zip(NAMES, rest)), hidden[...], rest[len(NAMES)])


def pair_kernel(keep, other, out):
    for i in range(4):
        rows = slice(i * 32, (i + 1) * 32)
        out[i] = (keep[rows, :] + other[rows, :].astype(F32)).astype(BF16)


def finish_kernel(arrived, own_rows, out):
    zl, y = lax.axis_index("zl"), lax.axis_index("y")
    for place, k in enumerate((0, 1, -1, 2, -2, 3, -3, 4)):
        block = lax.rem(zl + k + 8, 8)
        columns = pl.ds(pl.multiple_of(block * 256, 256), 256)
        total = jnp.zeros((32, 256), F32)
        for i in range(4):
            total = total + arrived[i, :, place * 256 : (place + 1) * 256].astype(F32)
        total = jnp.where(y % 2 == 1, pltpu.roll(total, 64, 1), total)
        total = jnp.where(y >= 2, pltpu.roll(total, 128, 1), total)
        out[:, columns] = (own_rows[:, columns] + total).astype(BF16)


def shards(
    stream, gain_mix, w_query, scale_query, w_key, scale_key, w_value, scale_value,
    gain_ffn, w_gate, scale_gate, w_up, scale_up, w_down, scale_down,
):
    hbm = pl.BlockSpec(memory_space=pltpu.HBM)
    qkv, ffn = call(
        pack_kernel,
        (jax.ShapeDtypeStruct((4, 64, 768), BF16), jax.ShapeDtypeStruct((96, 768), BF16)),
        *[
            pltpu.with_memory_space_constraint(array, pltpu.HBM)
            for array in (w_query, w_key, w_value, w_gate, w_up, w_down, scale_down[None])
        ],
        specs=[hbm] * 7,
        scratch=[pltpu.VMEM((64, n), F32) for n in (256, 256, 256, 352, 352, 352)]
        + [pltpu.VMEM((1, 64), F32), pltpu.SemaphoreType.DMA((7,))],
    )

    def rows_of(count):
        return jax.ShapeDtypeStruct((count, 768), BF16)

    fp1, fm1 = shift(ffn, Z, 1), shift(ffn, Z, -1)
    whole = lax.all_to_all(qkv, "y", split_axis=0, concat_axis=0, tiled=True).reshape(256, 768)
    own = call(first_plus_kernel, rows_of(352), whole, fp1)
    own_m = call(first_minus_kernel, rows_of(352), whole, fm1)
    p1, m1 = shift(own, Z, 1), shift(own_m, Z, -1)
    p2, m2 = shift(p1, Z, 1), shift(m1, Z, -1)
    angle = np.arange(LEN)[:, None] * THETA ** (-(np.arange(128) / 128))
    normed, tables, scales, wide, gain = call(
        early_kernel,
        tuple(
            jax.ShapeDtypeStruct(shape, kind)
            for shape, kind in (
                ((256, 2048), BF16), ((2, LEN, 128), F32), ((3, 1, 256), F32), ((2, 1, 384), F32), ((8, 1, 256), F32)
            )
        ),
        stream, gain_mix[None], jnp.asarray(np.cos(angle), F32), jnp.asarray(np.sin(angle), F32),
        scale_query[None], scale_key[None], scale_value[None], scale_gate[None], scale_up[None],
        gain_ffn.reshape(8, 1, 256), limit=12,
    )
    a0 = call(round_a_kernel, rows_of(480), ffn, fp1, fm1, p1, m1)
    ap, am = shift(a0, "y", 1), shift(a0, "y", -1)
    p3, m3 = shift(p2[0:304], Z, 1), shift(m2[0:304], Z, -1)
    b0 = call(round_b_kernel, rows_of(192), p2, m2)
    bp, bm = shift(b0, "y", 1), shift(b0, "y", -1)
    p4 = shift(p3[0:256], Z, 1)
    c0, c0_m, last = call(round_c_kernel, (rows_of(432), rows_of(432), rows_of(96)), p3, m3, bp, bm, ap, am)
    cp, cm = shift(c0, "y", 1), shift(c0_m, "y", -1)
    d2 = shift(last, "y", 2)

    mixed = call(
        retention_kernel,
        jax.ShapeDtypeStruct((4, 256, 256), BF16),
        normed, own, p1, m1, p2, m2, p3, m3, p4, scales, tables,
    )
    heads = lax.all_to_all(mixed, "x", split_axis=0, concat_axis=0, tiled=True)
    others = shift(heads, "c", 1)
    shards_of_ffn = (a0, ap, am, b0, bp, bm, c0, cp, cm, d2)
    own_resid, own_acc, own_total = call(
        ffn_own_kernel,
        tuple(jax.ShapeDtypeStruct(shape, F32) for shape in ((4, 256, 256), (256, 768), (256, 1))),
        stream, heads, gain, *shards_of_ffn, limit=12,
    )
    send, kept, own_rows = call(
        ffn_kernel,
        (
            jax.ShapeDtypeStruct((128, 2048), BF16),
            jax.ShapeDtypeStruct((128, 384), BF16),
            jax.ShapeDtypeStruct((32, 2048), F32),
        ),
        stream, others, gain, own_resid, own_acc, own_total, wide, *shards_of_ffn,
        scratch=[pltpu.VMEM((4, 256, 256), F32), pltpu.VMEM((256, 768), F32)],
        limit=12,
    )
    other = shift(send, "c", 1)
    keep = call(down_kernel, jax.ShapeDtypeStruct((128, 2048), F32), kept, *shards_of_ffn, limit=12)
    partial = call(pair_kernel, jax.ShapeDtypeStruct((4, 32, 2048), BF16), keep, other)
    arrived = lax.all_to_all(partial, "x", split_axis=0, concat_axis=0, tiled=True)
    return call(
        finish_kernel, jax.ShapeDtypeStruct((32, 2048), BF16), arrived, own_rows
    )


def solution(mesh):
    torus = Mesh(
        mesh.devices.reshape(mesh.shape["rep"], mesh.shape["fs"] // 4, 4, 4, 2),
        ("zh", "zl", "y", "x", "c"),
    )
    rows, weight, columns = P(("zh", "zl", "y"), None), P(("zl", "y"), TP), P(TP)
    in_specs = (
        rows, P(), weight, columns, weight, columns, weight, columns,
        P(), weight, columns, weight, columns, weight, P(("zl", "y")),
    )
    return jax.shard_map(
        shards, mesh=torus, in_specs=in_specs, out_specs=P(("zh", "zl", "y", "x", "c"), None), check_vma=False
    )
```
